128 devices in a mesh: ep: 128 (over z, y, x, core).
Axes of the slice: x: 4, y: 4, z: 4, core: 2. Of those that a mesh axis runs over, the one named last changes fastest.
Arguments:
- tokens: bfloat16 [4096, 2048], P('ep'), may hold values from -6 to 6
- gain_mix: float32 [2048], replicated, may hold values from 0.1 to 1.9
- w_query: bfloat16 [2048, 384], replicated, may hold values from -0.125 to 0.125
- w_key: bfloat16 [2048, 384], replicated, may hold values from -0.125 to 0.125
- w_value: bfloat16 [2048, 768], replicated, may hold values from -0.125 to 0.125
- w_input_gate: bfloat16 [2048, 4], replicated, may hold values from -0.125 to 0.125
- w_forget_gate: bfloat16 [2048, 4], replicated, may hold values from -0.125 to 0.125
- bias_input: float32 [4], replicated, may hold values from -1 to 1
- bias_forget: float32 [4], replicated, may hold values from 0 to 5
- memory_cells: float32 [4096, 4, 96, 192], P('ep'), may hold values from -6 to 6
- normalizer: float32 [4096, 4, 96], P('ep'), may hold values from -6 to 6
- stabilizer: float32 [4096, 4], P('ep'), may hold values from -1 to 1
- w_mix_out: bfloat16 [768, 2048], replicated, may hold values from -0.21875 to 0.21875
- gain_mix_post: float32 [2048], replicated, may hold values from 0.1 to 1.9
- gain_ffn: float32 [2048], replicated, may hold values from 0.1 to 1.9
- w_router: bfloat16 [2048, 32], replicated, may hold values from -0.125 to 0.125
- routing: int32 [4096, 2], replicated, may hold values from 0 to 31, all different within a row; in each aligned block of 32 rows (0 to 31, 32 to 63, ...) at most 4 rows name the same one
- w_expert_gate: bfloat16 [128, 2048, 384], P('ep'), may hold values from -0.125 to 0.125
- w_expert_up: bfloat16 [128, 2048, 384], P('ep'), may hold values from -0.125 to 0.125
- w_expert_down: bfloat16 [128, 384, 2048], P('ep'), may hold values from -0.15625 to 0.15625
- gain_ffn_post: float32 [2048], replicated, may hold values from 0.1 to 1.9
Outputs:
- mixed: bfloat16 [4096, 2048], P('ep')
- cells_next: float32 [4096, 4, 96, 192], P('ep')
- normalizer_next: float32 [4096, 4, 96], P('ep')
- stabilizer_next: float32 [4096, 4], P('ep')
The draws below stay inside these ranges and needn't reach their ends.
Inputs may be any that keep to these rules, and one draw needn't show every extreme that they name: `routing`: each row names 2 different experts. In the rows of one device (aligned blocks of 32 rows) no expert is named more than 4 times, a bound that some block reaches.
All inputs are finite; a program needn't handle non-finite values.
Results may differ from the reference program's by a relative error of at most 0.012.
Values may be sent and summed in bfloat16 or wider, within the bound.
A program may use at most 128 MiB of HBM per device.

```python
import math
import jax
import jax.numpy as jnp
import numpy as np
from jax import lax

D = 2048
HEADS = 4
DK = 96
DV = 192
FF_E = 1536
SPLIT = 4
TOP_K = 2
SEQ_DEV = 32
EXPERTS = 32
CAP = 4
TOKENS = 4096
N_EP = 128


def block_levels(stream_key, dims, split, smallest, largest):
    factor_of = 1.0
    for dim, parts in split:
        steps = jax.random.uniform(jax.random.fold_in(jax.random.fold_in(stream_key, 6), dim), (parts,), jnp.float32, smallest / len(split), largest / len(split))
        factor_of = factor_of * jnp.repeat(jnp.exp(steps), dims[dim] // parts).reshape((-1,) + (1,) * (len(dims) - 1 - dim))
    return factor_of


def routed_block(rng, own, number, rows, number_of, top, bound, lean):
    sequence = jax.random.permutation(rng, number_of)
    heavy_load, ordinary = shares(number_of, rows * top, bound, lean, True), shares(number_of, rows * top, bound, lean, False)
    places = jnp.arange(number_of)

    def named(tallies, offset_by):
        used = int((tallies > 0).sum())
        fixed = max(1, used // 4)
        passed = fixed + (places - fixed + offset_by * (used - fixed)) % max(1, number_of - fixed)
        return jnp.zeros((number_of,), jnp.int32).at[sequence[jnp.where(places < fixed, places, passed)]].set(jnp.asarray(tallies, jnp.int32))

    tallies = jnp.where(number % 4 == 0, named(heavy_load, number // 4), named(ordinary, number - number // 4 - 1))
    mixed = jax.random.permutation(jax.random.fold_in(own, 3), number_of)
    giver, sink = mixed[0:number_of // 2 * 2:2], mixed[1:number_of // 2 * 2:2]
    margin = jnp.minimum(tallies[giver] - 1, bound - tallies[sink]) // 2
    margin = jnp.where((giver == sequence[0]) | (sink == sequence[0]) | (tallies[sink] == 0), 0, jnp.maximum(margin, 0))
    passed = jax.random.randint(jax.random.fold_in(own, 4), (number_of // 2,), 0, 1 << 20) % (margin + 1)
    tallies = tallies.at[giver].add(-passed).at[sink].add(passed)
    members = jnp.searchsorted(jnp.cumsum(tallies), jnp.arange(rows * top), side="right").astype(jnp.int32)
    listing = members.reshape(top, rows).T
    listing = listing[jax.random.permutation(jax.random.fold_in(own, 1), rows)]
    offset_by = jax.random.randint(jax.random.fold_in(own, 2), (rows, 1), 0, top)
    return jnp.take_along_axis(listing, (jnp.arange(top)[None, :] + offset_by) % top, axis=1)


def shares(count, total, most, skew, full):
    portions = [(1 << 20) // math.isqrt(grade ** skew) + 1 for grade in range(1, count + 1)]
    largest = most if full else min(most, max(-(-total // count), total * portions[0] // sum(portions)))
    least = 1 if total - largest >= count - 1 else 0
    given, rest = [largest] + [least] * (count - 1), total - largest - least * (count - 1)
    while rest > 0:
        candidates = [i for i in range(1, count) if given[i] < largest] or [i for i in range(1, count) if given[i] < most]
        whole, budget = sum([portions[i] for i in candidates]), rest
        for i in candidates:
            extra = min(most - given[i], max(1, budget * portions[i] // whole), rest)
            given[i] = given[i] + extra
            rest = rest - extra
    return np.array(given)


def normal_values(own_key, dims, spread, limit, pieces=(), kind=jnp.bfloat16):
    values = spread * jax.random.normal(own_key, dims, jnp.float32)
    if pieces:
        values = values * block_levels(own_key, dims, pieces, -0.22, 0.18)
    return jnp.clip(values, -limit, limit).astype(kind)


def setup_inputs(seed: int = 0) -> dict:
    arg_keys = jax.random.split(jax.random.key(seed), 22)
    tokens = normal_values(arg_keys[0], (TOKENS, D), 1.0, 6.0, ((0, 128),))
    gain_mix = jnp.clip(1.0 + 0.18 * jax.random.normal(arg_keys[1], (D,), jnp.float32), 0.1, 1.9)
    w_query = normal_values(arg_keys[2], (D, HEADS * DK), D ** -0.5, 0.125)
    w_key = normal_values(arg_keys[3], (D, HEADS * DK), D ** -0.5, 0.125)
    w_value = normal_values(arg_keys[4], (D, HEADS * DV), D ** -0.5, 0.125)
    w_input_gate = normal_values(arg_keys[5], (D, HEADS), D ** -0.5, 0.125)
    w_forget_gate = normal_values(arg_keys[6], (D, HEADS), D ** -0.5, 0.125)
    bias_input = jnp.clip(jax.random.uniform(arg_keys[7], (HEADS,), jnp.float32, -1.0, 1.0), -1.0, 1.0)
    bias_forget = jnp.clip(jax.random.uniform(arg_keys[8], (HEADS,), jnp.float32, 0.0, 5.0), 0.0, 5.0)
    memory_cells = normal_values(arg_keys[9], (TOKENS, HEADS, DK, DV), 1.0, 6.0, ((0, 128),), jnp.float32)
    normalizer = normal_values(arg_keys[10], (TOKENS, HEADS, DK), 1.0, 6.0, ((0, 128),), jnp.float32)
    stabilizer = jnp.clip(jax.random.uniform(arg_keys[11], (TOKENS, HEADS), jnp.float32, -1.0, 1.0) * block_levels(arg_keys[11], (TOKENS, HEADS), ((0, 128),), -0.4, 0.0), -1.0, 1.0)
    w_mix_out = normal_values(arg_keys[12], (HEADS * DV, D), (HEADS * DV) ** -0.5, 0.21875)
    gain_mix_post = jnp.clip(1.0 + 0.18 * jax.random.normal(arg_keys[13], (D,), jnp.float32), 0.1, 1.9)
    gain_ffn = jnp.clip(1.0 + 0.18 * jax.random.normal(arg_keys[14], (D,), jnp.float32), 0.1, 1.9)
    w_router = normal_values(arg_keys[15], (D, EXPERTS), D ** -0.5, 0.125)
    routing_keys = jax.random.split(jax.random.fold_in(arg_keys[16], 1), TOKENS // SEQ_DEV)
    routing_turns = jax.random.permutation(jax.random.fold_in(arg_keys[16], 3), TOKENS // SEQ_DEV)
    routing = jax.vmap(lambda own, number: routed_block(jax.random.fold_in(arg_keys[16], 2), own, number, SEQ_DEV, EXPERTS, TOP_K, CAP, 2))(routing_keys, routing_turns).reshape((TOKENS, TOP_K))
    w_expert_gate = normal_values(arg_keys[17], (EXPERTS * SPLIT, D, FF_E // SPLIT), D ** -0.5, 0.125, ((0, 128),))
    w_expert_up = normal_values(arg_keys[18], (EXPERTS * SPLIT, D, FF_E // SPLIT), D ** -0.5, 0.125, ((0, 128),))
    w_expert_down = normal_values(arg_keys[19], (EXPERTS * SPLIT, FF_E // SPLIT, D), FF_E ** -0.5, 0.15625, ((0, 128),))
    gain_ffn_post = jnp.clip(1.0 + 0.18 * jax.random.normal(arg_keys[20], (D,), jnp.float32), 0.1, 1.9)
    return dict(tokens=tokens, gain_mix=gain_mix, w_query=w_query, w_key=w_key, w_value=w_value, w_input_gate=w_input_gate, w_forget_gate=w_forget_gate, bias_input=bias_input, bias_forget=bias_forget, memory_cells=memory_cells, normalizer=normalizer, stabilizer=stabilizer, w_mix_out=w_mix_out, gain_mix_post=gain_mix_post, gain_ffn=gain_ffn, w_router=w_router, routing=routing, w_expert_gate=w_expert_gate, w_expert_up=w_expert_up, w_expert_down=w_expert_down, gain_ffn_post=gain_ffn_post)


epsilon = 1e-06

def normalize(values, gain):
    return values * lax.rsqrt(lax.optimization_barrier(jnp.mean(values * values, axis=-1, keepdims=True)) + epsilon) * gain

def rounded(values):
    return lax.optimization_barrier(values.astype(jnp.bfloat16)).astype(jnp.float32)

def cell_step(normed, w_query, w_key, w_value, w_input_gate, w_forget_gate, bias_input, bias_forget, memory_cells, normalizer, stabilizer):
    row_count, heads, key_size, value_size = memory_cells.shape
    query_rows = rounded(jnp.dot(normed, w_query, preferred_element_type=jnp.float32))
    query_rows = query_rows.reshape(row_count, heads, key_size) * key_size ** (-0.5)
    key_rows = rounded(jnp.dot(normed, w_key, preferred_element_type=jnp.float32)).reshape(row_count, heads, key_size)
    value_rows = rounded(jnp.dot(normed, w_value, preferred_element_type=jnp.float32)).reshape(row_count, heads, value_size)
    input_gate = jnp.dot(normed, w_input_gate, preferred_element_type=jnp.float32) + bias_input
    log_forget = jax.nn.log_sigmoid(jnp.dot(normed, w_forget_gate, preferred_element_type=jnp.float32) + bias_forget)
    carried = log_forget + stabilizer
    stab_next = jnp.maximum(carried, input_gate)
    keep_weight = jnp.exp(carried - stab_next)
    write_weight = jnp.exp(input_gate - stab_next)
    scaled_keys = write_weight[:, :, None] * key_rows
    cells_next = keep_weight[:, :, None, None] * memory_cells + scaled_keys[:, :, :, None] * value_rows[:, :, None, :]
    norm_next = keep_weight[:, :, None] * normalizer + scaled_keys
    numerator = jnp.einsum('bhd,bhde->bhe', query_rows, cells_next, precision=lax.Precision.HIGHEST)
    denominator = jnp.einsum('bhd,bhd->bh', query_rows, norm_next, precision=lax.Precision.HIGHEST)
    denominator = jnp.maximum(jnp.abs(denominator), jnp.exp(-stab_next))
    cell_out = (numerator / denominator[:, :, None]).reshape(row_count, heads * value_size).astype(jnp.bfloat16)
    return (cell_out, cells_next, norm_next, stab_next)

def route_weights(rows_in, w_router, routes):
    logits = jnp.dot(rows_in, w_router, preferred_element_type=jnp.float32)
    onehot = routes[:, :, None] == jnp.arange(w_router.shape[1], dtype=jnp.int32)[None, None, :]
    chosen = lax.optimization_barrier(jnp.sum(jnp.where(onehot, logits[:, None, :], 0.0), axis=-1))
    return jax.nn.sigmoid(chosen - chosen[:, ::-1])

def expert_partial(row_block, gate_w, up_w, down_w):
    gate_part = jnp.dot(row_block, gate_w, preferred_element_type=jnp.float32)
    up_part = jnp.dot(row_block, up_w, preferred_element_type=jnp.float32)
    hidden = (jax.nn.silu(gate_part) * up_part).astype(jnp.bfloat16)
    return rounded(jnp.dot(hidden, down_w, preferred_element_type=jnp.float32))

def reference(tokens, gain_mix, w_query, w_key, w_value, w_input_gate, w_forget_gate, bias_input, bias_forget, memory_cells, normalizer, stabilizer, w_mix_out, gain_mix_post, gain_ffn, w_router, routing, w_expert_gate, w_expert_up, w_expert_down, gain_ffn_post):
    residual = tokens.astype(jnp.float32)
    normed = normalize(residual, gain_mix).astype(jnp.bfloat16)
    cell_out, cells_next, norm_next, stab_next = cell_step(normed, w_query, w_key, w_value, w_input_gate, w_forget_gate, bias_input, bias_forget, memory_cells, normalizer, stabilizer)
    mix_out = jnp.dot(cell_out, w_mix_out, preferred_element_type=jnp.float32)
    after_mix = (residual + normalize(mix_out, gain_mix_post)).astype(jnp.bfloat16)
    after_float = after_mix.astype(jnp.float32)
    expert_in = normalize(after_float, gain_ffn).astype(jnp.bfloat16)
    route_weight = route_weights(expert_in, w_router, routing)
    onehot = (routing[:, :, None] == jnp.arange(EXPERTS, dtype=jnp.int32)[None, None, :]).astype(jnp.int32)
    flat_hot = onehot.reshape(N_EP, SEQ_DEV * TOP_K, EXPERTS)
    slot_index = lax.optimization_barrier(jnp.sum((jnp.cumsum(flat_hot, axis=1) - 1) * flat_hot, axis=-1))
    position = (jnp.arange(N_EP, dtype=jnp.int32)[:, None] * CAP + slot_index).reshape(-1).astype(jnp.int32)
    expert_index = routing.reshape(-1).astype(jnp.int32)
    repeated = jnp.repeat(expert_in, TOP_K, axis=0)
    buffer = jnp.zeros((EXPERTS, N_EP * CAP, D), jnp.bfloat16).at[expert_index, position].set(repeated)
    quarter_width = FF_E // SPLIT
    gate_all = w_expert_gate.reshape(EXPERTS, SPLIT, D, quarter_width)
    up_all = w_expert_up.reshape(EXPERTS, SPLIT, D, quarter_width)
    down_all = w_expert_down.reshape(EXPERTS, SPLIT, quarter_width, D)

    def serve(operands):
        row_block, gate_w, up_w, down_w = operands
        running = jnp.zeros((row_block.shape[0], D), jnp.float32)
        for quarter_index in range(SPLIT):
            running = running + expert_partial(row_block, gate_w[quarter_index], up_w[quarter_index], down_w[quarter_index])
        return running
    results = lax.map(serve, (buffer, gate_all, up_all, down_all))
    picked = results[expert_index, position]
    expert_sum = lax.optimization_barrier(jnp.sum((picked * route_weight.reshape(-1, 1)).reshape(-1, TOP_K, D), axis=1))
    mixed = (after_float + normalize(expert_sum, gain_ffn_post)).astype(jnp.bfloat16)
    return (mixed, cells_next, norm_next, stab_next)
```

```python
import functools

import jax
import jax.numpy as jnp
from jax import lax
from jax.experimental import pallas as pl
from jax.experimental.pallas import tpu as pltpu
from jax.sharding import PartitionSpec as P

MESH = pl.DeviceIdType.MESH
F32, BF16 = jnp.float32, jnp.bfloat16
epsilon = 1e-06
VMEM_LIMIT = 64 * 1024 * 1024 - 64 * 1024

ROWS = 32
SLOTS = 4
CHIPS = 64
GROUPS = 4
PER = CHIPS // GROUPS
LANES = CHIPS * SLOTS
HALF = LANES // GROUPS
CHUNK = 4


def rms(values, gain):
    scale = lax.rsqrt(jnp.mean(values * values, axis=-1, keepdims=True) + epsilon)
    return values * scale * gain


def offset_of(index):
    g, dy, dx = index // PER, index // 4 % 4, index % 4
    return (g - dy - dx) % 4, dy, dx


def front_kernel(
    tok, gain_mix, wq, wk, wv, wi, wf, bias_i, bias_f, cells, norm, stab, wmix, gain_post, gain_ffn, wr, routes,
    cells_out, norm_out, stab_out, after_out, expert_out, weight_out, place_out,
    tok_v, gmix_v, wq_v, wk_v, wv_v, wi_v, wf_v, bi_v, bf_v, m_v, norm_v, stab_v, wmix_v, gpost_v, gffn_v, wr_v, rt_v,
    kt_v, qt_v, v_v, keep_v, write_v, num_v, den_v, t_v, in_sem, cell_sem, out_sem,
):
    me = lax.axis_index("ep")
    rows, heads, dk, dv = cells.shape
    chunks = rows // CHUNK
    t_v[...] = jnp.zeros_like(t_v)
    block = pl.multiple_of(me // 4 * 128, 128)
    pairs = [
        (tok, tok_v), (gain_mix, gmix_v), (wi, wi_v), (wf, wf_v), (bias_i, bi_v), (bias_f, bf_v), (stab, stab_v),
        (wq, wq_v), (wk, wk_v), (wv, wv_v), (norm, norm_v), (wmix, wmix_v), (gain_post, gpost_v), (gain_ffn, gffn_v),
        (wr, wr_v), (routes.at[:, pl.ds(block, 128)], rt_v),
    ]
    loads = [pltpu.make_async_copy(s, d, in_sem.at[i]) for i, (s, d) in enumerate(pairs)]

    def cell_load(ch):
        part = pl.ds(ch * CHUNK, CHUNK)
        return pltpu.make_async_copy(cells.at[part], m_v.at[part], cell_sem.at[ch])

    def cell_store(ch):
        part = pl.ds(ch * CHUNK, CHUNK)
        return pltpu.make_async_copy(m_v.at[part], cells_out.at[part], out_sem.at[ch])

    for copy in loads[:11]:
        copy.start()
    for ch in range(chunks):
        cell_load(ch).start()
    for copy in loads[11:]:
        copy.start()

    loads[0].wait()
    loads[1].wait()
    normed = rms(tok_v[...].astype(F32), gmix_v[...]).astype(BF16)

    for i in range(2, 7):
        loads[i].wait()
    nt = (((1,), (1,)), ((), ()))
    gate_in = lax.dot_general(normed, wi_v[...], nt, preferred_element_type=F32) + bi_v[...]
    forget = lax.dot_general(normed, wf_v[...], nt, preferred_element_type=F32) + bf_v[...]
    log_forget = jnp.minimum(forget, 0.0) - jnp.log1p(jnp.exp(-jnp.abs(forget)))
    t_v[0:heads, 0:rows] = stab_v[...]
    carried = log_forget + t_v[...].T[0:rows, 0:heads]
    stab_next = jnp.maximum(carried, gate_in)
    keep = jnp.exp(carried - stab_next)
    write = jnp.exp(gate_in - stab_next)
    floor = jnp.exp(-stab_next)
    for h in range(heads):
        keep_v[:, h, :] = jnp.broadcast_to(keep[:, h : h + 1], (rows, 128))
        write_v[:, h, :] = jnp.broadcast_to(write[:, h : h + 1], (rows, 128))
        t_v[0:rows, h : h + 1] = stab_next[:, h : h + 1]
    stab_out[...] = t_v[...].T[0:heads, 0:rows]

    loads[7].wait()
    query = jnp.dot(normed, wq_v[...], preferred_element_type=F32).astype(BF16).astype(F32)
    loads[8].wait()
    key = jnp.dot(normed, wk_v[...], preferred_element_type=F32).astype(BF16).astype(F32)
    pad = jnp.zeros((128 - rows, heads * dk), F32)
    qt_v[...] = jnp.concatenate([query, pad], axis=0).T
    kt_v[...] = jnp.concatenate([key, pad], axis=0).T
    loads[9].wait()
    value = jnp.dot(normed, wv_v[...], preferred_element_type=F32).astype(BF16).astype(F32)
    for h in range(heads):
        v_v[:, h, 0:dv] = value[:, dv * h : dv * h + dv]
    loads[10].wait()
    scale = dk ** (-0.5)
    for h in range(heads):
        fresh = keep[:, h : h + 1] * norm_v[:, h, :] + write[:, h : h + 1] * key[:, dk * h : dk * h + dk]
        norm_out[:, h, :] = fresh
        along = jnp.sum(query[:, dk * h : dk * h + dk] * scale * fresh, axis=-1, keepdims=True)
        den = jnp.maximum(jnp.abs(along), floor[:, h : h + 1])
        den_v[:, 128 * h : 128 * h + 128] = jnp.broadcast_to(den, (rows, 128))

    def serve(ch, carry):
        cell_load(ch).wait()
        shift = lax.rem(128 - ch * CHUNK, 128)
        for h in range(heads):
            kt = pltpu.roll(kt_v[dk * h : dk * h + dk, :], shift, 1)
            qt = pltpu.roll(qt_v[dk * h : dk * h + dk, :], shift, 1)
            for j in range(CHUNK):
                b = ch * CHUNK + j
                kc = jnp.broadcast_to(kt[:, j : j + 1], (dk, 128))
                qc = jnp.broadcast_to(qt[:, j : j + 1], (dk, 128))
                keep_b = keep_v[b, h : h + 1, :]
                write_b = write_v[b, h : h + 1, :]
                for lo, hi in ((0, 128), (128, dv)):
                    n = hi - lo
                    fed = write_b[:, :n] * v_v[b, h : h + 1, lo:hi]
                    fresh = keep_b[:, :n] * m_v[b, h, :, lo:hi] + kc[:, :n] * fed
                    m_v[b, h, :, lo:hi] = fresh
                    num_v[b, h : h + 1, lo:hi] = jnp.sum(qc[:, :n] * fresh, axis=0, keepdims=True)
        cell_store(ch).start()
        return carry

    lax.fori_loop(0, chunks, serve, 0)

    loads[11].wait()
    mix = jnp.zeros((rows, tok.shape[1]), F32)
    for h in range(heads):
        den = den_v[:, 128 * h : 128 * h + 128]
        wide = jnp.concatenate([den, den[:, : dv - 128]], axis=1)
        cell = (num_v[:, h, 0:dv] * scale / wide).astype(BF16)
        mix = mix + jnp.dot(cell, wmix_v[dv * h : dv * h + dv, :], preferred_element_type=F32)
    for i in range(12, 16):
        loads[i].wait()
    after = (tok_v[...].astype(F32) + rms(mix, gpost_v[...])).astype(BF16)
    after_out[...] = after
    expert_in = rms(after.astype(F32), gffn_v[...]).astype(BF16)
    expert_out[...] = expert_in

    t_v[...] = jnp.zeros_like(t_v)
    t_v[0:2, :] = rt_v[...].astype(F32)
    t_v[...] = t_v[...].T
    own = t_v[pl.ds(pl.multiple_of(lax.rem(me, 4) * rows, rows), rows), :]
    first, second = own[:, 0:1], own[:, 1:2]
    logits = lax.dot_general(expert_in, wr_v[...], nt, preferred_element_type=F32)
    ids = lax.broadcasted_iota(jnp.int32, logits.shape, 1).astype(F32)
    zero = jnp.zeros_like(logits)
    chosen0 = jnp.sum(jnp.where(ids == first, logits, zero), axis=-1, keepdims=True)
    chosen1 = jnp.sum(jnp.where(ids == second, logits, zero), axis=-1, keepdims=True)
    weight0 = jax.nn.sigmoid(chosen0 - chosen1)
    weight1 = jax.nn.sigmoid(chosen1 - chosen0)
    lane = lax.broadcasted_iota(jnp.int32, (rows, LANES), 1)
    index = lane >> 2
    dy, dx = (index >> 2) & 3, index & 3
    dz = ((index >> 4) - dy - dx + 8) & 3
    mine = me // 2
    cz = (mine // 16 + dz) & 3
    cy = (lax.rem(mine // 4, 4) + dy) & 3
    cx = (lax.rem(mine, 4) + dx) & 3
    expert = ((cz * 16 + cy * 4 + cx) >> 1).astype(F32)
    hit0 = (expert == first).astype(F32)
    hit1 = (expert == second).astype(F32)
    hot = hit0 + hit1
    before = lax.broadcasted_iota(jnp.int32, (rows, rows), 1) < lax.broadcasted_iota(jnp.int32, (rows, rows), 0)
    rank = jnp.dot(before.astype(F32).astype(BF16), hot.astype(BF16), preferred_element_type=F32)
    place = jnp.where(rank == (lane & 3).astype(F32), hot, 0.0)
    place_out[...] = place.astype(BF16)
    weight_out[...] = place * (hit0 * weight0 + hit1 * weight1)

    def drain(ch, carry):
        cell_store(ch).wait()
        return carry

    lax.fori_loop(0, chunks, drain, 0)


def expert_kernel(
    expert_in, after, weight, place, wg, wu, wd, gain_post,
    mixed,
    wg_v, wu_v, wd_v, send, xa, xb, own_part, part_send, part_recv, back_send, back,
    w_sem, send_s, send_r, fwd_s, fwd_r, part_s, part_r, back_s, back_r,
):
    me = lax.axis_index("ep")
    core, chip = lax.rem(me, 2), me // 2
    z, y, x = chip // 16, lax.rem(chip // 4, 4), lax.rem(chip, 4)
    partner = me + 1 - 2 * core

    def at(index, sign):
        dz, dy, dx = offset_of(index)
        if sign < 0:
            dz, dy, dx = -dz % 4, -dy % 4, -dx % 4
        return ((lax.rem(z + dz, 4) * 4 + lax.rem(y + dy, 4)) * 4 + lax.rem(x + dx, 4)) * 2 + core

    def cut(index):
        return pl.ds(SLOTS * index, SLOTS)

    barrier = pltpu.get_barrier_semaphore()
    for i in range(1, CHIPS):
        pl.semaphore_signal(barrier, inc=1, device_id=(at(i, 1),), device_id_type=MESH)
    pl.semaphore_signal(barrier, inc=1, device_id=(partner,), device_id_type=MESH)
    weights = [
        pltpu.make_async_copy(s.at[0], d, w_sem.at[i]) for i, (s, d) in enumerate(((wg, wg_v), (wu, wu_v), (wd, wd_v)))
    ]
    for copy in weights:
        copy.start()
    tn = (((0,), (0,)), ((), ()))
    send[...] = lax.dot_general(place[...], expert_in[...], tn, preferred_element_type=F32).astype(BF16)
    xa[0:SLOTS, :] = send[0:SLOTS, :]
    pl.semaphore_wait(barrier, CHIPS)

    def to_expert(i):
        return pltpu.make_async_remote_copy(
            src_ref=send.at[cut(i)], dst_ref=xa.at[cut(i)], send_sem=send_s.at[i], recv_sem=send_r.at[i],
            device_id=(at(i, 1),), device_id_type=MESH,
        )

    def to_source(i):
        return pltpu.make_async_remote_copy(
            src_ref=back_send.at[cut(i)], dst_ref=back.at[cut(i)], send_sem=back_s.at[i], recv_sem=back_r.at[i],
            device_id=(at(i, -1),), device_id_type=MESH,
        )

    def to_partner(src, dst, ssem, rsem, g):
        part = pl.ds(HALF * g, HALF)
        return pltpu.make_async_remote_copy(
            src_ref=src.at[part], dst_ref=dst.at[part], send_sem=ssem.at[g], recv_sem=rsem.at[g],
            device_id=(partner,), device_id_type=MESH,
        )

    order = list(range(GROUPS))[1:] + [0]
    for g in order:
        for i in range(PER * g, PER * g + PER):
            if i:
                to_expert(i).start()
    for copy in weights:
        copy.wait()

    def finish(g):
        part = slice(HALF * g, HALF * g + HALF)
        to_partner(part_send, part_recv, part_s, part_r, g).wait_recv()
        back_send[part, :] = (own_part[part, :] + part_recv[part, :].astype(F32)).astype(BF16)
        for i in range(PER * g, PER * g + PER):
            if i:
                to_source(i).start()
            else:
                back[0:SLOTS, :] = back_send[0:SLOTS, :]

    last = None
    for g in order:
        part = slice(HALF * g, HALF * g + HALF)
        for i in range(PER * g, PER * g + PER):
            if i:
                to_expert(i).wait_recv()
        to_partner(xa, xb, fwd_s, fwd_r, g).start()
        if last is not None:
            finish(last)
        to_partner(xa, xb, fwd_s, fwd_r, g).wait_recv()
        block = jnp.concatenate([xa[part, :], xb[part, :]], axis=0)
        gate = jnp.dot(block, wg_v[...], preferred_element_type=F32)
        up = jnp.dot(block, wu_v[...], preferred_element_type=F32)
        hidden = (gate * jax.nn.sigmoid(gate) * up).astype(BF16)
        result = jnp.dot(hidden, wd_v[...], preferred_element_type=F32)
        part_send[part, :] = result[HALF:, :].astype(BF16)
        to_partner(part_send, part_recv, part_s, part_r, g).start()
        own_part[part, :] = result[:HALF, :]
        last = g
    finish(last)

    total = None
    high = weight[...].astype(BF16)
    low = (weight[...] - high.astype(F32)).astype(BF16)
    for g in order:
        part = slice(HALF * g, HALF * g + HALF)
        for i in range(PER * g, PER * g + PER):
            if i:
                to_source(i).wait_recv()
        rows = back[part, :]
        more = jnp.dot(high[:, part], rows, preferred_element_type=F32)
        more = more + jnp.dot(low[:, part], rows, preferred_element_type=F32)
        total = more if total is None else total + more
    mixed[...] = (after[...].astype(F32) + rms(total, gain_post[...])).astype(BF16)

    for i in range(1, CHIPS):
        to_expert(i).wait_send()
        to_source(i).wait_send()
    for g in range(GROUPS):
        to_partner(xa, xb, fwd_s, fwd_r, g).wait_send()
        to_partner(part_send, part_recv, part_s, part_r, g).wait_send()


def body(
    tokens, gain_mix, w_query, w_key, w_value, w_input_gate, w_forget_gate, bias_input, bias_forget, memory_cells,
    normalizer, stabilizer, w_mix_out, gain_mix_post, gain_ffn, w_router, routing, w_expert_gate, w_expert_up,
    w_expert_down, gain_ffn_post,
):
    rows, width = tokens.shape
    _, heads, dk, dv = memory_cells.shape
    hidden = w_expert_gate.shape[2]
    row = lambda v: v.reshape(1, -1)
    front_in = (
        tokens, row(gain_mix), w_query, w_key, w_value, w_input_gate.T, w_forget_gate.T, row(bias_input),
        row(bias_forget), memory_cells, normalizer, stabilizer.T, w_mix_out, row(gain_mix_post), row(gain_ffn),
        w_router.T, routing.T,
    )
    anywhere, vmem = pl.BlockSpec(memory_space=pl.ANY), pl.BlockSpec(memory_space=pltpu.VMEM)
    shape = jax.ShapeDtypeStruct
    dma = pltpu.SemaphoreType.DMA
    scratch = [pltpu.VMEM(a.shape, a.dtype) for a in front_in]
    scratch[-1] = pltpu.VMEM((2, 128), jnp.int32)
    cells_next, norm_next, stab_next, after, expert_in, weight, place = pl.pallas_call(
        front_kernel,
        out_shape=(
            shape(memory_cells.shape, F32), shape(normalizer.shape, F32), shape((heads, rows), F32),
            shape((rows, width), BF16), shape((rows, width), BF16), shape((rows, LANES), F32), shape((rows, LANES), BF16),
        ),
        in_specs=[anywhere] * len(front_in),
        out_specs=(anywhere,) + (vmem,) * 6,
        scratch_shapes=scratch
        + [
            pltpu.VMEM((heads * dk, 128), F32), pltpu.VMEM((heads * dk, 128), F32), pltpu.VMEM((rows, heads, 256), F32),
            pltpu.VMEM((rows, heads, 128), F32), pltpu.VMEM((rows, heads, 128), F32),
            pltpu.VMEM((rows, heads, 256), F32), pltpu.VMEM((rows, heads * 128), F32), pltpu.VMEM((128, 128), F32),
            dma((16,)), dma((rows // CHUNK,)), dma((rows // CHUNK,)),
        ],
        compiler_params=pltpu.CompilerParams(vmem_limit_bytes=VMEM_LIMIT),
        name="front",
    )(*front_in)

    big = pltpu.VMEM((LANES, width), BF16)
    mixed = pl.pallas_call(
        expert_kernel,
        out_shape=shape((rows, width), BF16),
        in_specs=[vmem] * 4 + [anywhere] * 3 + [vmem],
        out_specs=vmem,
        scratch_shapes=[
            pltpu.VMEM((width, hidden), BF16), pltpu.VMEM((width, hidden), BF16), pltpu.VMEM((hidden, width), BF16),
            big, big, big, pltpu.VMEM((LANES, width), F32), big, big, big, big,
            dma((3,)), dma((CHIPS,)), dma((CHIPS,)), dma((GROUPS,)), dma((GROUPS,)), dma((GROUPS,)), dma((GROUPS,)),
            dma((CHIPS,)), dma((CHIPS,)),
        ],
        compiler_params=pltpu.CompilerParams(collective_id=0, has_side_effects=True, vmem_limit_bytes=VMEM_LIMIT),
        name="experts",
    )(expert_in, after, weight, place, w_expert_gate, w_expert_up, w_expert_down, row(gain_ffn_post))
    return (mixed, cells_next, norm_next, stab_next.T)


def solution(mesh):
    return jax.shard_map(
        body,
        mesh=mesh,
        in_specs=(
            P("ep", None),
            P(),
            P(),
            P(),
            P(),
            P(),
            P(),
            P(),
            P(),
            P("ep", None, None, None),
            P("ep", None, None),
            P("ep", None),
            P(),
            P(),
            P(),
            P(),
            P(),
            P("ep", None, None),
            P("ep", None, None),
            P("ep", None, None),
            P(),
        ),
        out_specs=(P("ep", None), P("ep", None, None, None), P("ep", None, None), P("ep", None)),
        check_vma=False,
    )
```

```python
import functools

import jax
import jax.numpy as jnp
from jax import lax
from jax.experimental import pallas as pl
from jax.experimental.pallas import tpu as pltpu
from jax.sharding import PartitionSpec as P

MESH = pl.DeviceIdType.MESH
F32, BF16 = jnp.float32, jnp.bfloat16
epsilon = 1e-06
VMEM_LIMIT = 64 * 1024 * 1024 - 256 * 1024

ROWS = 32
SLOTS = 4
CHIPS = 64
GROUPS = 4
PER = CHIPS // GROUPS
LANES = CHIPS * SLOTS
HALF = LANES // GROUPS
NT = (((1,), (1,)), ((), ()))
CHUNK = 4


def rms(values, gain):
    scale = lax.rsqrt(jnp.mean(values * values, axis=-1, keepdims=True) + epsilon)
    return values * scale * gain


def offset_of(index):
    g, dy, dx = index // PER, index // 4 % 4, index % 4
    return (g - dy - dx) % 4, dy, dx


def front_kernel(
    tok, gain_mix, wq, wk, wv, wi, wf, bias_i, bias_f, cells, norm, stab,
    cells_out, norm_out, stab_out, cell_out,
    tok_v, gmix_v, wq_v, wk_v, wv_v, wi_v, wf_v, bi_v, bf_v, m_v, norm_v, stab_v,
    cell_v, kt_v, q_v, v_v, keep_v, write_v, num_v, den_v, t_v, in_sem, cell_sem, out_sem,
):
    rows, heads, dk, dv = cells.shape
    chunks = rows // CHUNK
    pairs = [
        (tok, tok_v), (gain_mix, gmix_v), (wi, wi_v), (wf, wf_v), (bias_i, bi_v), (bias_f, bf_v), (stab, stab_v),
        (wq, wq_v), (wk, wk_v), (wv, wv_v), (norm, norm_v),
    ]
    loads = [pltpu.make_async_copy(s, d, in_sem.at[i]) for i, (s, d) in enumerate(pairs)]

    def cell_load(ch):
        part = pl.ds(ch * CHUNK, CHUNK)
        return pltpu.make_async_copy(cells.at[part], m_v.at[part], cell_sem.at[ch])

    def cell_store(ch):
        part = pl.ds(ch * CHUNK, CHUNK)
        return pltpu.make_async_copy(m_v.at[part], cells_out.at[part], out_sem.at[ch])

    for copy in loads:
        copy.start()
    cell_load(0).start()

    t_v[...] = jnp.zeros_like(t_v)
    loads[0].wait()
    loads[1].wait()
    normed = rms(tok_v[...].astype(F32), gmix_v[...]).astype(BF16)

    for i in range(2, 7):
        loads[i].wait()
    gate_in = lax.dot_general(normed, wi_v[...], NT, preferred_element_type=F32) + bi_v[...]
    forget = lax.dot_general(normed, wf_v[...], NT, preferred_element_type=F32) + bf_v[...]
    log_forget = jnp.minimum(forget, 0.0) - jnp.log1p(jnp.exp(-jnp.abs(forget)))
    t_v[0:heads, 0:rows] = stab_v[...]
    carried = log_forget + t_v[...].T[0:rows, 0:heads]
    stab_next = jnp.maximum(carried, gate_in)
    keep = jnp.exp(carried - stab_next)
    write = jnp.exp(gate_in - stab_next)
    floor = jnp.exp(-stab_next)
    for h in range(heads):
        keep_v[:, h, :] = jnp.broadcast_to(keep[:, h : h + 1], (rows, 128))
        write_v[:, h, :] = jnp.broadcast_to(write[:, h : h + 1], (rows, 128))
        t_v[0:rows, h : h + 1] = stab_next[:, h : h + 1]
    stab_out[...] = t_v[...].T[0:heads, 0:rows]

    loads[7].wait()
    for ch in range(1, 3):
        cell_load(ch).start()
    query = jnp.dot(normed, wq_v[...], preferred_element_type=F32).astype(BF16).astype(F32)
    loads[8].wait()
    for ch in range(3, chunks):
        cell_load(ch).start()
    key = jnp.dot(normed, wk_v[...], preferred_element_type=F32).astype(BF16).astype(F32)
    pad = jnp.zeros((128 - rows, heads * dk), F32)
    kt_v[...] = jnp.concatenate([key, pad], axis=0).T
    loads[9].wait()
    value = jnp.dot(normed, wv_v[...], preferred_element_type=F32).astype(BF16).astype(F32)
    for h in range(heads):
        v_v[:, h, 0:dv] = value[:, dv * h : dv * h + dv]
        for ch in range(chunks):
            q_v[ch, h, 0:CHUNK, 0:dk] = query[ch * CHUNK : ch * CHUNK + CHUNK, dk * h : dk * h + dk]
    loads[10].wait()
    scale = dk ** (-0.5)
    for h in range(heads):
        fresh = keep[:, h : h + 1] * norm_v[:, h, :] + write[:, h : h + 1] * key[:, dk * h : dk * h + dk]
        norm_out[:, h, :] = fresh
        along = jnp.sum(query[:, dk * h : dk * h + dk] * scale * fresh, axis=-1, keepdims=True)
        den = jnp.maximum(jnp.abs(along), floor[:, h : h + 1])
        den_v[:, 128 * h : 128 * h + 128] = jnp.broadcast_to(den, (rows, 128))

    def serve(ch, carry):
        cell_load(ch).wait()
        shift = lax.rem(128 - ch * CHUNK, 128)
        for h in range(heads):
            kt = pltpu.roll(kt_v[dk * h : dk * h + dk, :], shift, 1)
            q = q_v[ch, h, :, 0:dk].astype(BF16)
            for j in range(CHUNK):
                b = ch * CHUNK + j
                kc = jnp.broadcast_to(kt[:, j : j + 1], (dk, 128))
                keep_b = keep_v[b, h : h + 1, :]
                write_b = write_v[b, h : h + 1, :]
                parts = []
                for lo, hi in ((0, 128), (128, dv)):
                    n = hi - lo
                    fed = write_b[:, :n] * v_v[b, h : h + 1, lo:hi]
                    fresh = keep_b[:, :n] * m_v[b, h, :, lo:hi] + kc[:, :n] * fed
                    m_v[b, h, :, lo:hi] = fresh
                    parts.append(fresh)
                fresh = jnp.concatenate(parts, axis=1)
                high = fresh.astype(BF16)
                low = (fresh - high.astype(F32)).astype(BF16)
                num = jnp.dot(q, high, preferred_element_type=F32) + jnp.dot(q, low, preferred_element_type=F32)
                num_v[b, h : h + 1, 0:dv] = num[j : j + 1, :]
        cell_store(ch).start()
        return carry

    lax.fori_loop(0, chunks, serve, 0)
    for h in range(heads):
        den = den_v[:, 128 * h : 128 * h + 128]
        wide = jnp.concatenate([den, den[:, : dv - 128]], axis=1)
        cell_v[h, :, :] = (num_v[:, h, 0:dv] * scale / wide).astype(BF16)
    given = pltpu.make_async_copy(cell_v, cell_out, in_sem.at[11])
    given.start()

    def drain(ch, carry):
        cell_store(ch).wait()
        return carry

    lax.fori_loop(0, chunks, drain, 0)
    given.wait()


def expert_kernel(
    cell, tok, wmix, gain_post, gain_ffn, wr, routes, wg, wu, wd, gain_last,
    mixed,
    cell_v, tok_v, wmix_v, gpost_v, gffn_v, wr_v, rt_v, glast_v, t_v, wg_v, wu_v, wd_v, send, xa, xb, own_part, part_send, part_recv, back_send, back,
    in_sem, send_s, send_r, fwd_s, fwd_r, part_s, part_r, back_s, back_r,
):
    me = lax.axis_index("ep")
    core, chip = lax.rem(me, 2), me // 2
    z, y, x = chip // 16, lax.rem(chip // 4, 4), lax.rem(chip, 4)
    partner = me + 1 - 2 * core

    def at(index, sign):
        dz, dy, dx = offset_of(index)
        if sign < 0:
            dz, dy, dx = -dz % 4, -dy % 4, -dx % 4
        return ((lax.rem(z + dz, 4) * 4 + lax.rem(y + dy, 4)) * 4 + lax.rem(x + dx, 4)) * 2 + core

    def cut(index):
        return pl.ds(SLOTS * index, SLOTS)

    barrier = pltpu.get_barrier_semaphore()
    for i in range(1, CHIPS):
        pl.semaphore_signal(barrier, inc=1, device_id=(at(i, 1),), device_id_type=MESH)
    pl.semaphore_signal(barrier, inc=1, device_id=(partner,), device_id_type=MESH)
    block = pl.multiple_of(me // 4 * 128, 128)
    pairs = [
        (tok, tok_v), (routes.at[:, pl.ds(block, 128)], rt_v), (wmix, wmix_v), (gain_post, gpost_v), (gain_ffn, gffn_v),
        (wr, wr_v), (gain_last, glast_v), (cell, cell_v), (wg.at[0], wg_v), (wu.at[0], wu_v), (wd.at[0], wd_v),
    ]
    loads = [pltpu.make_async_copy(s, d, in_sem.at[i]) for i, (s, d) in enumerate(pairs)]
    for copy in loads[:8]:
        copy.start()

    loads[0].wait()
    loads[1].wait()
    rows, (heads, _, dv) = tok_v.shape[0], cell.shape
    t_v[...] = jnp.zeros_like(t_v)
    t_v[0:2, :] = rt_v[...].astype(F32)
    t_v[...] = t_v[...].T
    own = t_v[pl.ds(pl.multiple_of(lax.rem(me, 4) * rows, rows), rows), :]
    first, second = own[:, 0:1], own[:, 1:2]
    lane = lax.broadcasted_iota(jnp.int32, (rows, LANES), 1)
    index = lane >> 2
    dy, dx = (index >> 2) & 3, index & 3
    dz = ((index >> 4) - dy - dx + 8) & 3
    expert = ((((z + dz) & 3) * 16 + ((y + dy) & 3) * 4 + ((x + dx) & 3)) >> 1).astype(F32)
    hit0 = (expert == first).astype(F32)
    hit1 = (expert == second).astype(F32)
    hot = hit0 + hit1
    before = lax.broadcasted_iota(jnp.int32, (rows, rows), 1) < lax.broadcasted_iota(jnp.int32, (rows, rows), 0)
    rank = jnp.dot(before.astype(F32).astype(BF16), hot.astype(BF16), preferred_element_type=F32)
    place = jnp.where(rank == (lane & 3).astype(F32), hot, 0.0)

    loads[2].wait()
    loads[7].wait()
    for copy in loads[8:]:
        copy.start()
    mix = jnp.zeros(tok_v.shape, F32)
    for h in range(heads):
        mix = mix + jnp.dot(cell_v[h], wmix_v[dv * h : dv * h + dv, :], preferred_element_type=F32)
    for i in range(3, 7):
        loads[i].wait()
    after = (tok_v[...].astype(F32) + rms(mix, gpost_v[...])).astype(BF16).astype(F32)
    expert_in = rms(after, gffn_v[...]).astype(BF16)
    tn = (((0,), (0,)), ((), ()))
    send[...] = lax.dot_general(place.astype(BF16), expert_in, tn, preferred_element_type=F32).astype(BF16)
    xa[0:SLOTS, :] = send[0:SLOTS, :]
    pl.semaphore_wait(barrier, CHIPS)

    def to_expert(i):
        return pltpu.make_async_remote_copy(
            src_ref=send.at[cut(i)], dst_ref=xa.at[cut(i)], send_sem=send_s.at[i], recv_sem=send_r.at[i],
            device_id=(at(i, 1),), device_id_type=MESH,
        )

    def to_source(i):
        return pltpu.make_async_remote_copy(
            src_ref=back_send.at[cut(i)], dst_ref=back.at[cut(i)], send_sem=back_s.at[i], recv_sem=back_r.at[i],
            device_id=(at(i, -1),), device_id_type=MESH,
        )

    def to_partner(src, dst, ssem, rsem, g):
        part = pl.ds(HALF * g, HALF)
        return pltpu.make_async_remote_copy(
            src_ref=src.at[part], dst_ref=dst.at[part], send_sem=ssem.at[g], recv_sem=rsem.at[g],
            device_id=(partner,), device_id_type=MESH,
        )

    order = list(range(GROUPS))[1:] + [0]
    for g in order:
        for i in range(PER * g, PER * g + PER):
            if i:
                to_expert(i).start()

    logits = lax.dot_general(expert_in, wr_v[...], NT, preferred_element_type=F32)
    ids = lax.broadcasted_iota(jnp.int32, logits.shape, 1).astype(F32)
    zero = jnp.zeros_like(logits)
    chosen0 = jnp.sum(jnp.where(ids == first, logits, zero), axis=-1, keepdims=True)
    chosen1 = jnp.sum(jnp.where(ids == second, logits, zero), axis=-1, keepdims=True)
    weight = place * (hit0 * jax.nn.sigmoid(chosen0 - chosen1) + hit1 * jax.nn.sigmoid(chosen1 - chosen0))
    high = weight.astype(BF16)
    low = (weight - high.astype(F32)).astype(BF16)
    for copy in loads[8:]:
        copy.wait()

    def finish(g):
        part = slice(HALF * g, HALF * g + HALF)
        to_partner(part_send, part_recv, part_s, part_r, g).wait_recv()
        back_send[part, :] = (own_part[part, :] + part_recv[part, :].astype(F32)).astype(BF16)
        for i in range(PER * g, PER * g + PER):
            if i:
                to_source(i).start()
            else:
                back[0:SLOTS, :] = back_send[0:SLOTS, :]

    last = None
    for g in order:
        part = slice(HALF * g, HALF * g + HALF)
        for i in range(PER * g, PER * g + PER):
            if i:
                to_expert(i).wait_recv()
        to_partner(xa, xb, fwd_s, fwd_r, g).start()
        if last is not None:
            finish(last)
        to_partner(xa, xb, fwd_s, fwd_r, g).wait_recv()
        block = jnp.concatenate([xa[part, :], xb[part, :]], axis=0)
        gate = jnp.dot(block, wg_v[...], preferred_element_type=F32)
        up = jnp.dot(block, wu_v[...], preferred_element_type=F32)
        hidden = (gate * jax.nn.sigmoid(gate) * up).astype(BF16)
        result = jnp.dot(hidden, wd_v[...], preferred_element_type=F32)
        part_send[part, :] = result[HALF:, :].astype(BF16)
        to_partner(part_send, part_recv, part_s, part_r, g).start()
        own_part[part, :] = result[:HALF, :]
        last = g
    finish(last)

    total = None
    for g in order:
        part = slice(HALF * g, HALF * g + HALF)
        for i in range(PER * g, PER * g + PER):
            if i:
                to_source(i).wait_recv()
        rows = back[part, :]
        more = jnp.dot(high[:, part], rows, preferred_element_type=F32)
        more = more + jnp.dot(low[:, part], rows, preferred_element_type=F32)
        total = more if total is None else total + more
    mixed[...] = (after + rms(total, glast_v[...])).astype(BF16)

    for i in range(1, CHIPS):
        to_expert(i).wait_send()
        to_source(i).wait_send()
    for g in range(GROUPS):
        to_partner(xa, xb, fwd_s, fwd_r, g).wait_send()
        to_partner(part_send, part_recv, part_s, part_r, g).wait_send()


def body(
    tokens, gain_mix, w_query, w_key, w_value, w_input_gate, w_forget_gate, bias_input, bias_forget, memory_cells,
    normalizer, stabilizer, w_mix_out, gain_mix_post, gain_ffn, w_router, routing, w_expert_gate, w_expert_up,
    w_expert_down, gain_ffn_post,
):
    rows, width = tokens.shape
    _, heads, dk, dv = memory_cells.shape
    hidden = w_expert_gate.shape[2]
    row = lambda v: v.reshape(1, -1)
    hbm, vmem = pl.BlockSpec(memory_space=pltpu.HBM), pl.BlockSpec(memory_space=pltpu.VMEM)
    shape = jax.ShapeDtypeStruct
    dma = pltpu.SemaphoreType.DMA
    like = lambda a: pltpu.VMEM(a.shape, a.dtype)
    front_in = (
        tokens, row(gain_mix), w_query, w_key, w_value, w_input_gate.T, w_forget_gate.T, row(bias_input),
        row(bias_forget), memory_cells, normalizer, stabilizer.T,
    )
    cells_next, norm_next, stab_next, cell = pl.pallas_call(
        front_kernel,
        out_shape=(
            shape(memory_cells.shape, F32), shape(normalizer.shape, F32), shape((heads, rows), F32),
            shape((heads, rows, dv), BF16),
        ),
        in_specs=[hbm] * len(front_in),
        out_specs=(hbm, vmem, vmem, hbm),
        scratch_shapes=[like(a) for a in front_in]
        + [
            pltpu.VMEM((heads, rows, dv), BF16),
            pltpu.VMEM((heads * dk, 128), F32), pltpu.VMEM((rows // CHUNK, heads, 8, 128), F32),
            pltpu.VMEM((rows, heads, 256), F32), pltpu.VMEM((rows, heads, 128), F32), pltpu.VMEM((rows, heads, 128), F32),
            pltpu.VMEM((rows, heads, 256), F32), pltpu.VMEM((rows, heads * 128), F32), pltpu.VMEM((128, 128), F32),
            dma((12,)), dma((rows // CHUNK,)), dma((rows // CHUNK,)),
        ],
        compiler_params=pltpu.CompilerParams(vmem_limit_bytes=VMEM_LIMIT),
        name="front",
    )(*front_in)

    big = pltpu.VMEM((LANES, width), BF16)
    router = w_router.T
    mixed = pl.pallas_call(
        expert_kernel,
        out_shape=pltpu.VMEM((rows, width), BF16),
        in_specs=[hbm] * 11,
        out_specs=vmem,
        scratch_shapes=[
            pltpu.VMEM((heads, rows, dv), BF16), like(tokens), like(w_mix_out), like(row(gain_mix_post)), like(row(gain_ffn)), like(router),
            pltpu.VMEM((2, 128), jnp.int32), like(row(gain_ffn_post)), pltpu.VMEM((128, 128), F32),
            pltpu.VMEM((width, hidden), BF16), pltpu.VMEM((width, hidden), BF16), pltpu.VMEM((hidden, width), BF16),
            big, big, big, pltpu.VMEM((LANES, width), F32), big, big, big, big,
            dma((11,)), dma((CHIPS,)), dma((CHIPS,)), dma((GROUPS,)), dma((GROUPS,)), dma((GROUPS,)), dma((GROUPS,)),
            dma((CHIPS,)), dma((CHIPS,)),
        ],
        compiler_params=pltpu.CompilerParams(collective_id=0, has_side_effects=True, vmem_limit_bytes=VMEM_LIMIT - 256 * 1024),
        name="experts",
    )(
        cell, tokens, w_mix_out, row(gain_mix_post), row(gain_ffn), router, routing.T, w_expert_gate, w_expert_up,
        w_expert_down, row(gain_ffn_post),
    )
    return (mixed, cells_next, norm_next, stab_next.T)


def solution(mesh):
    return jax.shard_map(
        body,
        mesh=mesh,
        in_specs=(
            P("ep", None),
            P(),
            P(),
            P(),
            P(),
            P(),
            P(),
            P(),
            P(),
            P("ep", None, None, None),
            P("ep", None, None),
            P("ep", None),
            P(),
            P(),
            P(),
            P(),
            P(),
            P("ep", None, None),
            P("ep", None, None),
            P("ep", None, None),
            P(),
        ),
        out_specs=(P("ep", None), P("ep", None, None, None), P("ep", None, None), P("ep", None)),
        check_vma=False,
    )
```

```python
import functools

import jax
import jax.numpy as jnp
from jax import lax
from jax.experimental import pallas as pl
from jax.experimental.pallas import tpu as pltpu
from jax.sharding import PartitionSpec as P

MESH = pl.DeviceIdType.MESH
F32, BF16 = jnp.float32, jnp.bfloat16
epsilon = 1e-06
VMEM_LIMIT = 64 * 1024 * 1024 - 256 * 1024

ROWS = 32
SLOTS = 4
CHIPS = 64
GROUPS = 4
PER = CHIPS // GROUPS
LANES = CHIPS * SLOTS
HALF = LANES // GROUPS
NT = (((1,), (1,)), ((), ()))
CHUNK = 8


def rms(values, gain):
    scale = lax.rsqrt(jnp.mean(values * values, axis=-1, keepdims=True) + epsilon)
    return values * scale * gain


def offset_of(index):
    g, dy, dx = index // PER, index // 4 % 4, index % 4
    return (g - dy - dx) % 4, dy, dx


def hops(index):
    return sum(min(v, 4 - v) for v in offset_of(index))


def front_kernel(
    tok, gain_mix, wq, wk, wv, wi, wf, bias_i, bias_f, cells, norm, stab,
    cells_out, norm_out, stab_out, cell_out,
    tok_v, gmix_v, wq_v, wk_v, wv_v, wi_v, wf_v, bi_v, bf_v, m_v, norm_v, stab_v,
    cell_v, kt_v, q_v, v_v, keep_v, write_v, num_v, den_v, t_v, in_sem, cell_sem, out_sem,
):
    rows, heads, dk, dv = cells.shape
    chunks = rows // CHUNK
    pairs = [
        (tok, tok_v), (gain_mix, gmix_v), (wi, wi_v), (wf, wf_v), (bias_i, bi_v), (bias_f, bf_v), (stab, stab_v),
        (wq, wq_v), (wk, wk_v), (wv, wv_v), (norm, norm_v),
    ]
    loads = [pltpu.make_async_copy(s, d, in_sem.at[i]) for i, (s, d) in enumerate(pairs)]

    def cell_load(ch):
        part = pl.ds(ch * CHUNK, CHUNK)
        return pltpu.make_async_copy(cells.at[part], m_v.at[part], cell_sem.at[ch])

    def cell_store(ch):
        part = pl.ds(ch * CHUNK, CHUNK)
        return pltpu.make_async_copy(m_v.at[part], cells_out.at[part], out_sem.at[ch])

    for copy in loads:
        copy.start()
    cell_load(0).start()

    t_v[...] = jnp.zeros_like(t_v)
    loads[0].wait()
    loads[1].wait()
    normed = rms(tok_v[...].astype(F32), gmix_v[...]).astype(BF16)

    for i in range(2, 7):
        loads[i].wait()
    gate_in = lax.dot_general(normed, wi_v[...], NT, preferred_element_type=F32) + bi_v[...]
    forget = lax.dot_general(normed, wf_v[...], NT, preferred_element_type=F32) + bf_v[...]
    log_forget = jnp.minimum(forget, 0.0) - jnp.log1p(jnp.exp(-jnp.abs(forget)))
    t_v[0:heads, 0:rows] = stab_v[...]
    carried = log_forget + t_v[...].T[0:rows, 0:heads]
    stab_next = jnp.maximum(carried, gate_in)
    keep = jnp.exp(carried - stab_next)
    write = jnp.exp(gate_in - stab_next)
    floor = jnp.exp(-stab_next)
    for h in range(heads):
        keep_v[:, h, :] = jnp.broadcast_to(keep[:, h : h + 1], (rows, 128))
        write_v[:, h, :] = jnp.broadcast_to(write[:, h : h + 1], (rows, 128))
        t_v[0:rows, h : h + 1] = stab_next[:, h : h + 1]
    stab_out[...] = t_v[...].T[0:heads, 0:rows]

    loads[7].wait()
    for ch in range(1, 2):
        cell_load(ch).start()
    query = jnp.dot(normed, wq_v[...], preferred_element_type=F32).astype(BF16).astype(F32)
    loads[8].wait()
    for ch in range(2, chunks):
        cell_load(ch).start()
    key = jnp.dot(normed, wk_v[...], preferred_element_type=F32).astype(BF16).astype(F32)
    pad = jnp.zeros((128 - rows, heads * dk), F32)
    kt_v[...] = jnp.concatenate([key, pad], axis=0).T
    loads[9].wait()
    value = jnp.dot(normed, wv_v[...], preferred_element_type=F32).astype(BF16).astype(F32)
    for h in range(heads):
        v_v[:, h, 0:dv] = value[:, dv * h : dv * h + dv]
        for ch in range(chunks):
            q_v[ch, h, 0:CHUNK, 0:dk] = query[ch * CHUNK : ch * CHUNK + CHUNK, dk * h : dk * h + dk]
    loads[10].wait()
    scale = dk ** (-0.5)
    for h in range(heads):
        fresh = keep[:, h : h + 1] * norm_v[:, h, :] + write[:, h : h + 1] * key[:, dk * h : dk * h + dk]
        norm_out[:, h, :] = fresh
        along = jnp.sum(query[:, dk * h : dk * h + dk] * scale * fresh, axis=-1, keepdims=True)
        den = jnp.maximum(jnp.abs(along), floor[:, h : h + 1])
        den_v[:, 128 * h : 128 * h + 128] = jnp.broadcast_to(den, (rows, 128))

    def serve(ch, carry):
        cell_load(ch).wait()
        shift = lax.rem(128 - ch * CHUNK, 128)
        for h in range(heads):
            kt = pltpu.roll(kt_v[dk * h : dk * h + dk, :], shift, 1)
            q = q_v[ch, h, :, 0:dk].astype(BF16)
            for j in range(CHUNK):
                b = ch * CHUNK + j
                kc = jnp.broadcast_to(kt[:, j : j + 1], (dk, 128))
                keep_b = keep_v[b, h : h + 1, :]
                write_b = write_v[b, h : h + 1, :]
                parts = []
                for lo, hi in ((0, 128), (128, dv)):
                    n = hi - lo
                    fed = write_b[:, :n] * v_v[b, h : h + 1, lo:hi]
                    fresh = keep_b[:, :n] * m_v[b, h, :, lo:hi] + kc[:, :n] * fed
                    m_v[b, h, :, lo:hi] = fresh
                    parts.append(fresh)
                fresh = jnp.concatenate(parts, axis=1)
                high = fresh.astype(BF16)
                low = (fresh - high.astype(F32)).astype(BF16)
                num = jnp.dot(q, high, preferred_element_type=F32) + jnp.dot(q, low, preferred_element_type=F32)
                num_v[b, h : h + 1, 0:dv] = num[j : j + 1, :]
        cell_store(ch).start()
        return carry

    lax.fori_loop(0, chunks, serve, 0)
    for h in range(heads):
        den = den_v[:, 128 * h : 128 * h + 128]
        wide = jnp.concatenate([den, den[:, : dv - 128]], axis=1)
        cell_v[h, :, :] = (num_v[:, h, 0:dv] * scale / wide).astype(BF16)
    given = pltpu.make_async_copy(cell_v, cell_out, in_sem.at[11])
    given.start()

    def drain(ch, carry):
        cell_store(ch).wait()
        return carry

    lax.fori_loop(0, chunks, drain, 0)
    given.wait()


def expert_kernel(
    cell, tok, wmix, gain_post, gain_ffn, wr, routes, wg, wu, wd, gain_last,
    mixed,
    cell_v, tok_v, wmix_v, gpost_v, gffn_v, wr_v, rt_v, glast_v, t_v, wg_v, wu_v, wd_v, send, xa, xb, own_part, part_send, part_recv, back_send, back,
    in_sem, send_s, send_r, fwd_s, fwd_r, part_s, part_r, back_s, back_r,
):
    me = lax.axis_index("ep")
    core, chip = lax.rem(me, 2), me // 2
    z, y, x = chip // 16, lax.rem(chip // 4, 4), lax.rem(chip, 4)
    partner = me + 1 - 2 * core

    def at(index, sign):
        dz, dy, dx = offset_of(index)
        if sign < 0:
            dz, dy, dx = -dz % 4, -dy % 4, -dx % 4
        return ((lax.rem(z + dz, 4) * 4 + lax.rem(y + dy, 4)) * 4 + lax.rem(x + dx, 4)) * 2 + core

    def cut(index):
        return pl.ds(SLOTS * index, SLOTS)

    barrier = pltpu.get_barrier_semaphore()
    for i in sorted(range(1, CHIPS), key=lambda i: -hops(i)):
        pl.semaphore_signal(barrier, inc=1, device_id=(at(i, 1),), device_id_type=MESH)
    pl.semaphore_signal(barrier, inc=1, device_id=(partner,), device_id_type=MESH)
    block = pl.multiple_of(me // 4 * 128, 128)
    pairs = [
        (tok, tok_v), (routes.at[:, pl.ds(block, 128)], rt_v), (wmix, wmix_v), (gain_post, gpost_v), (gain_ffn, gffn_v),
        (wr, wr_v), (gain_last, glast_v), (cell, cell_v), (wg.at[0], wg_v), (wu.at[0], wu_v), (wd.at[0], wd_v),
    ]
    loads = [pltpu.make_async_copy(s, d, in_sem.at[i]) for i, (s, d) in enumerate(pairs)]
    for copy in loads[:8]:
        copy.start()

    loads[0].wait()
    loads[1].wait()
    rows, (heads, _, dv) = tok_v.shape[0], cell.shape
    t_v[...] = jnp.zeros_like(t_v)
    t_v[0:2, :] = rt_v[...].astype(F32)
    t_v[...] = t_v[...].T
    own = t_v[pl.ds(pl.multiple_of(lax.rem(me, 4) * rows, rows), rows), :]
    first, second = own[:, 0:1], own[:, 1:2]
    lane = lax.broadcasted_iota(jnp.int32, (rows, LANES), 1)
    index = lane >> 2
    dy, dx = (index >> 2) & 3, index & 3
    dz = ((index >> 4) - dy - dx + 8) & 3
    expert = ((((z + dz) & 3) * 16 + ((y + dy) & 3) * 4 + ((x + dx) & 3)) >> 1).astype(F32)
    hit0 = (expert == first).astype(F32)
    hit1 = (expert == second).astype(F32)
    hot = hit0 + hit1
    before = lax.broadcasted_iota(jnp.int32, (rows, rows), 1) < lax.broadcasted_iota(jnp.int32, (rows, rows), 0)
    rank = jnp.dot(before.astype(F32).astype(BF16), hot.astype(BF16), preferred_element_type=F32)
    place = jnp.where(rank == (lane & 3).astype(F32), hot, 0.0)

    loads[2].wait()
    loads[7].wait()
    for copy in loads[8:]:
        copy.start()
    mix = jnp.zeros(tok_v.shape, F32)
    for h in range(heads):
        mix = mix + jnp.dot(cell_v[h], wmix_v[dv * h : dv * h + dv, :], preferred_element_type=F32)
    for i in range(3, 7):
        loads[i].wait()
    after = (tok_v[...].astype(F32) + rms(mix, gpost_v[...])).astype(BF16).astype(F32)
    expert_in = rms(after, gffn_v[...]).astype(BF16)
    tn = (((0,), (0,)), ((), ()))
    send[...] = lax.dot_general(place.astype(BF16), expert_in, tn, preferred_element_type=F32).astype(BF16)
    xa[0:SLOTS, :] = send[0:SLOTS, :]
    pl.semaphore_wait(barrier, CHIPS)

    def to_expert(i):
        return pltpu.make_async_remote_copy(
            src_ref=send.at[cut(i)], dst_ref=xa.at[cut(i)], send_sem=send_s.at[i], recv_sem=send_r.at[i],
            device_id=(at(i, 1),), device_id_type=MESH,
        )

    def to_source(i):
        return pltpu.make_async_remote_copy(
            src_ref=back_send.at[cut(i)], dst_ref=back.at[cut(i)], send_sem=back_s.at[i], recv_sem=back_r.at[i],
            device_id=(at(i, -1),), device_id_type=MESH,
        )

    def to_partner(src, dst, ssem, rsem, g):
        part = pl.ds(HALF * g, HALF)
        return pltpu.make_async_remote_copy(
            src_ref=src.at[part], dst_ref=dst.at[part], send_sem=ssem.at[g], recv_sem=rsem.at[g],
            device_id=(partner,), device_id_type=MESH,
        )

    order = [2, 1, 3, 0]
    for g in order:
        for i in sorted(range(PER * g, PER * g + PER), key=lambda i: -hops(i)):
            if i:
                to_expert(i).start()

    logits = lax.dot_general(expert_in, wr_v[...], NT, preferred_element_type=F32)
    ids = lax.broadcasted_iota(jnp.int32, logits.shape, 1).astype(F32)
    zero = jnp.zeros_like(logits)
    chosen0 = jnp.sum(jnp.where(ids == first, logits, zero), axis=-1, keepdims=True)
    chosen1 = jnp.sum(jnp.where(ids == second, logits, zero), axis=-1, keepdims=True)
    weight = place * (hit0 * jax.nn.sigmoid(chosen0 - chosen1) + hit1 * jax.nn.sigmoid(chosen1 - chosen0))
    high = weight.astype(BF16)
    low = (weight - high.astype(F32)).astype(BF16)
    for copy in loads[8:]:
        copy.wait()

    def finish(g):
        part = slice(HALF * g, HALF * g + HALF)
        to_partner(part_send, part_recv, part_s, part_r, g).wait_recv()
        back_send[part, :] = (own_part[part, :] + part_recv[part, :].astype(F32)).astype(BF16)
        for i in range(PER * g, PER * g + PER):
            if i:
                to_source(i).start()
            else:
                back[0:SLOTS, :] = back_send[0:SLOTS, :]

    last = None
    for g in order:
        part = slice(HALF * g, HALF * g + HALF)
        for i in range(PER * g, PER * g + PER):
            if i:
                to_expert(i).wait_recv()
        to_partner(xa, xb, fwd_s, fwd_r, g).start()
        if last is not None:
            finish(last)
        to_partner(xa, xb, fwd_s, fwd_r, g).wait_recv()
        block = jnp.concatenate([xa[part, :], xb[part, :]], axis=0)
        gate = jnp.dot(block, wg_v[...], preferred_element_type=F32)
        up = jnp.dot(block, wu_v[...], preferred_element_type=F32)
        hidden = (gate * jax.nn.sigmoid(gate) * up).astype(BF16)
        result = jnp.dot(hidden, wd_v[...], preferred_element_type=F32)
        part_send[part, :] = result[HALF:, :].astype(BF16)
        to_partner(part_send, part_recv, part_s, part_r, g).start()
        own_part[part, :] = result[:HALF, :]
        last = g
    finish(last)

    total = None
    for g in order:
        part = slice(HALF * g, HALF * g + HALF)
        for i in range(PER * g, PER * g + PER):
            if i:
                to_source(i).wait_recv()
        rows = back[part, :]
        more = jnp.dot(high[:, part], rows, preferred_element_type=F32)
        more = more + jnp.dot(low[:, part], rows, preferred_element_type=F32)
        total = more if total is None else total + more
    mixed[...] = (after + rms(total, glast_v[...])).astype(BF16)

    for i in range(1, CHIPS):
        to_expert(i).wait_send()
        to_source(i).wait_send()
    for g in range(GROUPS):
        to_partner(xa, xb, fwd_s, fwd_r, g).wait_send()
        to_partner(part_send, part_recv, part_s, part_r, g).wait_send()


def body(
    tokens, gain_mix, w_query, w_key, w_value, w_input_gate, w_forget_gate, bias_input, bias_forget, memory_cells,
    normalizer, stabilizer, w_mix_out, gain_mix_post, gain_ffn, w_router, routing, w_expert_gate, w_expert_up,
    w_expert_down, gain_ffn_post,
):
    rows, width = tokens.shape
    _, heads, dk, dv = memory_cells.shape
    hidden = w_expert_gate.shape[2]
    row = lambda v: v.reshape(1, -1)
    hbm, vmem = pl.BlockSpec(memory_space=pltpu.HBM), pl.BlockSpec(memory_space=pltpu.VMEM)
    shape = jax.ShapeDtypeStruct
    dma = pltpu.SemaphoreType.DMA
    like = lambda a: pltpu.VMEM(a.shape, a.dtype)
    front_in = (
        tokens, row(gain_mix), w_query, w_key, w_value, w_input_gate.T, w_forget_gate.T, row(bias_input),
        row(bias_forget), memory_cells, normalizer, stabilizer.T,
    )
    cells_next, norm_next, stab_next, cell = pl.pallas_call(
        front_kernel,
        out_shape=(
            shape(memory_cells.shape, F32), shape(normalizer.shape, F32), shape((heads, rows), F32),
            shape((heads, rows, dv), BF16),
        ),
        in_specs=[hbm] * len(front_in),
        out_specs=(hbm, vmem, vmem, hbm),
        scratch_shapes=[like(a) for a in front_in]
        + [
            pltpu.VMEM((heads, rows, dv), BF16),
            pltpu.VMEM((heads * dk, 128), F32), pltpu.VMEM((rows // CHUNK, heads, 8, 128), F32),
            pltpu.VMEM((rows, heads, 256), F32), pltpu.VMEM((rows, heads, 128), F32), pltpu.VMEM((rows, heads, 128), F32),
            pltpu.VMEM((rows, heads, 256), F32), pltpu.VMEM((rows, heads * 128), F32), pltpu.VMEM((128, 128), F32),
            dma((12,)), dma((rows // CHUNK,)), dma((rows // CHUNK,)),
        ],
        compiler_params=pltpu.CompilerParams(vmem_limit_bytes=VMEM_LIMIT),
        name="front",
    )(*front_in)

    big = pltpu.VMEM((LANES, width), BF16)
    router = w_router.T
    mixed = pl.pallas_call(
        expert_kernel,
        out_shape=pltpu.VMEM((rows, width), BF16),
        in_specs=[hbm] * 11,
        out_specs=vmem,
        scratch_shapes=[
            pltpu.VMEM((heads, rows, dv), BF16), like(tokens), like(w_mix_out), like(row(gain_mix_post)), like(row(gain_ffn)), like(router),
            pltpu.VMEM((2, 128), jnp.int32), like(row(gain_ffn_post)), pltpu.VMEM((128, 128), F32),
            pltpu.VMEM((width, hidden), BF16), pltpu.VMEM((width, hidden), BF16), pltpu.VMEM((hidden, width), BF16),
            big, big, big, pltpu.VMEM((LANES, width), F32), big, big, big, big,
            dma((11,)), dma((CHIPS,)), dma((CHIPS,)), dma((GROUPS,)), dma((GROUPS,)), dma((GROUPS,)), dma((GROUPS,)),
            dma((CHIPS,)), dma((CHIPS,)),
        ],
        compiler_params=pltpu.CompilerParams(collective_id=0, has_side_effects=True, vmem_limit_bytes=VMEM_LIMIT - 256 * 1024),
        name="experts",
    )(
        cell, tokens, w_mix_out, row(gain_mix_post), row(gain_ffn), router, routing.T, w_expert_gate, w_expert_up,
        w_expert_down, row(gain_ffn_post),
    )
    return (mixed, cells_next, norm_next, stab_next.T)


def solution(mesh):
    return jax.shard_map(
        body,
        mesh=mesh,
        in_specs=(
            P("ep", None),
            P(),
            P(),
            P(),
            P(),
            P(),
            P(),
            P(),
            P(),
            P("ep", None, None, None),
            P("ep", None, None),
            P("ep", None),
            P(),
            P(),
            P(),
            P(),
            P(),
            P("ep", None, None),
            P("ep", None, None),
            P("ep", None, None),
            P(),
        ),
        out_specs=(P("ep", None), P("ep", None, None, None), P("ep", None, None), P("ep", None)),
        check_vma=False,
    )
```

```python
import functools

import jax
import jax.numpy as jnp
from jax import lax
from jax.experimental import pallas as pl
from jax.experimental.pallas import tpu as pltpu
from jax.sharding import PartitionSpec as P

MESH = pl.DeviceIdType.MESH
F32, BF16 = jnp.float32, jnp.bfloat16
epsilon = 1e-06
VMEM_LIMIT = 64 * 1024 * 1024 - 256 * 1024

ROWS = 32
SLOTS = 4
CHIPS = 64
GROUPS = 4
PER = CHIPS // GROUPS
LANES = CHIPS * SLOTS
HALF = LANES // GROUPS
NT = (((1,), (1,)), ((), ()))
CHUNK = 8


def rms(values, gain):
    scale = lax.rsqrt(jnp.mean(values * values, axis=-1, keepdims=True) + epsilon)
    return values * scale * gain


def offset_of(index):
    g, dy, dx = index // PER, index // 4 % 4, index % 4
    return (g - dy - dx) % 4, dy, dx


def hops(index):
    return sum(min(v, 4 - v) for v in offset_of(index))


def front_kernel(
    tok, gain_mix, wq, wk, wv, wi, wf, bias_i, bias_f, cells, norm, stab,
    cells_out, norm_out, stab_out, cell_out,
    tok_v, gmix_v, wq_v, wk_v, wv_v, wi_v, wf_v, bi_v, bf_v, m_v, norm_v, stab_v,
    cell_v, kt_v, q_v, v_v, keep_v, write_v, num_v, den_v, t_v, in_sem, cell_sem, out_sem,
):
    rows, heads, dk, dv = cells.shape
    chunks = rows // CHUNK
    pairs = [
        (tok, tok_v), (gain_mix, gmix_v), (wi, wi_v), (wf, wf_v), (bias_i, bi_v), (bias_f, bf_v), (stab, stab_v),
        (wq, wq_v), (wk, wk_v), (wv, wv_v), (norm, norm_v),
    ]
    loads = [pltpu.make_async_copy(s, d, in_sem.at[i]) for i, (s, d) in enumerate(pairs)]

    def cell_load(ch):
        part = pl.ds(ch * CHUNK, CHUNK)
        return pltpu.make_async_copy(cells.at[part], m_v.at[part], cell_sem.at[ch])

    def cell_store(ch):
        part = pl.ds(ch * CHUNK, CHUNK)
        return pltpu.make_async_copy(m_v.at[part], cells_out.at[part], out_sem.at[ch])

    for copy in loads:
        copy.start()
    cell_load(0).start()

    t_v[...] = jnp.zeros_like(t_v)
    loads[0].wait()
    loads[1].wait()
    normed = rms(tok_v[...].astype(F32), gmix_v[...]).astype(BF16)

    for i in range(2, 7):
        loads[i].wait()
    gate_in = lax.dot_general(normed, wi_v[...], NT, preferred_element_type=F32) + bi_v[...]
    forget = lax.dot_general(normed, wf_v[...], NT, preferred_element_type=F32) + bf_v[...]
    log_forget = jnp.minimum(forget, 0.0) - jnp.log1p(jnp.exp(-jnp.abs(forget)))
    t_v[0:heads, 0:rows] = stab_v[...]
    carried = log_forget + t_v[...].T[0:rows, 0:heads]
    stab_next = jnp.maximum(carried, gate_in)
    keep = jnp.exp(carried - stab_next)
    write = jnp.exp(gate_in - stab_next)
    floor = jnp.exp(-stab_next)
    for h in range(heads):
        keep_v[:, h, :] = jnp.broadcast_to(keep[:, h : h + 1], (rows, 128))
        write_v[:, h, :] = jnp.broadcast_to(write[:, h : h + 1], (rows, 128))
        t_v[0:rows, h : h + 1] = stab_next[:, h : h + 1]
    stab_out[...] = t_v[...].T[0:heads, 0:rows]

    loads[7].wait()
    for ch in range(1, 2):
        cell_load(ch).start()
    query = jnp.dot(normed, wq_v[...], preferred_element_type=F32).astype(BF16).astype(F32)
    loads[8].wait()
    for ch in range(2, chunks):
        cell_load(ch).start()
    key = jnp.dot(normed, wk_v[...], preferred_element_type=F32).astype(BF16).astype(F32)
    pad = jnp.zeros((128 - rows, heads * dk), F32)
    kt_v[...] = jnp.concatenate([key, pad], axis=0).T
    loads[9].wait()
    value = jnp.dot(normed, wv_v[...], preferred_element_type=F32).astype(BF16).astype(F32)
    for h in range(heads):
        v_v[:, h, 0:dv] = value[:, dv * h : dv * h + dv]
        for ch in range(chunks):
            q_v[ch, h, 0:CHUNK, 0:dk] = query[ch * CHUNK : ch * CHUNK + CHUNK, dk * h : dk * h + dk]
    loads[10].wait()
    scale = dk ** (-0.5)
    for h in range(heads):
        fresh = keep[:, h : h + 1] * norm_v[:, h, :] + write[:, h : h + 1] * key[:, dk * h : dk * h + dk]
        norm_out[:, h, :] = fresh
        along = jnp.sum(query[:, dk * h : dk * h + dk] * scale * fresh, axis=-1, keepdims=True)
        den = jnp.maximum(jnp.abs(along), floor[:, h : h + 1])
        den_v[:, 128 * h : 128 * h + 128] = jnp.broadcast_to(den, (rows, 128))

    def serve(ch, carry):
        cell_load(ch).wait()
        shift = lax.rem(128 - ch * CHUNK, 128)
        for h in range(heads):
            kt = pltpu.roll(kt_v[dk * h : dk * h + dk, :], shift, 1)
            q = q_v[ch, h, :, 0:dk].astype(BF16)
            for j in range(CHUNK):
                b = ch * CHUNK + j
                kc = jnp.broadcast_to(kt[:, j : j + 1], (dk, 128))
                keep_b = keep_v[b, h : h + 1, :]
                write_b = write_v[b, h : h + 1, :]
                parts = []
                for lo, hi in ((0, 128), (128, dv)):
                    n = hi - lo
                    fed = write_b[:, :n] * v_v[b, h : h + 1, lo:hi]
                    fresh = keep_b[:, :n] * m_v[b, h, :, lo:hi] + kc[:, :n] * fed
                    m_v[b, h, :, lo:hi] = fresh
                    parts.append(fresh)
                fresh = jnp.concatenate(parts, axis=1)
                high = fresh.astype(BF16)
                low = (fresh - high.astype(F32)).astype(BF16)
                num = jnp.dot(q, high, preferred_element_type=F32) + jnp.dot(q, low, preferred_element_type=F32)
                num_v[b, h : h + 1, 0:dv] = num[j : j + 1, :]
        cell_store(ch).start()
        return carry

    lax.fori_loop(0, chunks, serve, 0)
    for h in range(heads):
        den = den_v[:, 128 * h : 128 * h + 128]
        wide = jnp.concatenate([den, den[:, : dv - 128]], axis=1)
        cell_v[h, :, :] = (num_v[:, h, 0:dv] * scale / wide).astype(BF16)
    given = pltpu.make_async_copy(cell_v, cell_out, in_sem.at[11])
    given.start()

    def drain(ch, carry):
        cell_store(ch).wait()
        return carry

    lax.fori_loop(0, chunks, drain, 0)
    given.wait()


def expert_kernel(
    cell, tok, wmix, gain_post, gain_ffn, wr, routes, wg, wu, wd, gain_last,
    mixed,
    cell_v, tok_v, wmix_v, gpost_v, gffn_v, wr_v, rt_v, glast_v, t_v, wg_v, wu_v, wd_v, send, xa, xb, own_part, part_send, part_recv, back_send, back,
    in_sem, send_s, send_r, fwd_s, fwd_r, part_s, part_r, back_s, back_r,
):
    me = lax.axis_index("ep")
    core, chip = lax.rem(me, 2), me // 2
    z, y, x = chip // 16, lax.rem(chip // 4, 4), lax.rem(chip, 4)
    partner = me + 1 - 2 * core

    def at(index, sign):
        dz, dy, dx = offset_of(index)
        if sign < 0:
            dz, dy, dx = -dz % 4, -dy % 4, -dx % 4
        return ((lax.rem(z + dz, 4) * 4 + lax.rem(y + dy, 4)) * 4 + lax.rem(x + dx, 4)) * 2 + core

    def cut(index):
        return pl.ds(SLOTS * index, SLOTS)

    barrier = pltpu.get_barrier_semaphore()
    for i in sorted(range(1, CHIPS), key=lambda i: -hops(i)):
        pl.semaphore_signal(barrier, inc=1, device_id=(at(i, 1),), device_id_type=MESH)
    pl.semaphore_signal(barrier, inc=1, device_id=(partner,), device_id_type=MESH)
    block = pl.multiple_of(me // 4 * 128, 128)
    pairs = [
        (tok, tok_v), (routes.at[:, pl.ds(block, 128)], rt_v), (wmix, wmix_v), (gain_post, gpost_v), (gain_ffn, gffn_v),
        (wr, wr_v), (gain_last, glast_v), (cell, cell_v), (wg.at[0], wg_v), (wu.at[0], wu_v), (wd.at[0], wd_v),
    ]
    loads = [pltpu.make_async_copy(s, d, in_sem.at[i]) for i, (s, d) in enumerate(pairs)]
    for copy in loads[:8]:
        copy.start()

    loads[0].wait()
    loads[1].wait()
    rows, (heads, _, dv) = tok_v.shape[0], cell.shape
    t_v[...] = jnp.zeros_like(t_v)
    t_v[0:2, :] = rt_v[...].astype(F32)
    t_v[...] = t_v[...].T
    own = t_v[pl.ds(pl.multiple_of(lax.rem(me, 4) * rows, rows), rows), :]
    first, second = own[:, 0:1], own[:, 1:2]
    lane = lax.broadcasted_iota(jnp.int32, (rows, LANES), 1)
    index = lane >> 2
    dy, dx = (index >> 2) & 3, index & 3
    dz = ((index >> 4) - dy - dx + 8) & 3
    expert = ((((z + dz) & 3) * 16 + ((y + dy) & 3) * 4 + ((x + dx) & 3)) >> 1).astype(F32)
    hit0 = (expert == first).astype(F32)
    hit1 = (expert == second).astype(F32)
    hot = hit0 + hit1
    before = lax.broadcasted_iota(jnp.int32, (rows, rows), 1) < lax.broadcasted_iota(jnp.int32, (rows, rows), 0)
    rank = jnp.dot(before.astype(F32).astype(BF16), hot.astype(BF16), preferred_element_type=F32)
    place = jnp.where(rank == (lane & 3).astype(F32), hot, 0.0)

    loads[2].wait()
    loads[7].wait()
    for copy in loads[8:]:
        copy.start()
    mix = jnp.zeros(tok_v.shape, F32)
    for h in range(heads):
        mix = mix + jnp.dot(cell_v[h], wmix_v[dv * h : dv * h + dv, :], preferred_element_type=F32)
    for i in range(3, 7):
        loads[i].wait()
    after = (tok_v[...].astype(F32) + rms(mix, gpost_v[...])).astype(BF16).astype(F32)
    expert_in = rms(after, gffn_v[...]).astype(BF16)
    tn = (((0,), (0,)), ((), ()))
    send[...] = lax.dot_general(place.astype(BF16), expert_in, tn, preferred_element_type=F32).astype(BF16)
    xa[0:SLOTS, :] = send[0:SLOTS, :]
    pl.semaphore_wait(barrier, CHIPS)

    def to_expert(i):
        return pltpu.make_async_remote_copy(
            src_ref=send.at[cut(i)], dst_ref=xa.at[cut(i)], send_sem=send_s.at[i], recv_sem=send_r.at[i],
            device_id=(at(i, 1),), device_id_type=MESH,
        )

    def to_source(i):
        return pltpu.make_async_remote_copy(
            src_ref=back_send.at[cut(i)], dst_ref=back.at[cut(i)], send_sem=back_s.at[i], recv_sem=back_r.at[i],
            device_id=(at(i, -1),), device_id_type=MESH,
        )

    def to_partner(src, dst, ssem, rsem, g):
        part = pl.ds(HALF * g, HALF)
        return pltpu.make_async_remote_copy(
            src_ref=src.at[part], dst_ref=dst.at[part], send_sem=ssem.at[g], recv_sem=rsem.at[g],
            device_id=(partner,), device_id_type=MESH,
        )

    order = [2, 1, 3, 0]
    for g in order:
        for i in sorted(range(PER * g, PER * g + PER), key=lambda i: -hops(i)):
            if i:
                to_expert(i).start()

    logits = lax.dot_general(expert_in, wr_v[...], NT, preferred_element_type=F32)
    ids = lax.broadcasted_iota(jnp.int32, logits.shape, 1).astype(F32)
    zero = jnp.zeros_like(logits)
    chosen0 = jnp.sum(jnp.where(ids == first, logits, zero), axis=-1, keepdims=True)
    chosen1 = jnp.sum(jnp.where(ids == second, logits, zero), axis=-1, keepdims=True)
    weight = place * (hit0 * jax.nn.sigmoid(chosen0 - chosen1) + hit1 * jax.nn.sigmoid(chosen1 - chosen0))
    high = weight.astype(BF16)
    low = (weight - high.astype(F32)).astype(BF16)
    for copy in loads[8:]:
        copy.wait()

    def finish(g):
        part = slice(HALF * g, HALF * g + HALF)
        to_partner(part_send, part_recv, part_s, part_r, g).wait_recv()
        back_send[part, :] = (own_part[part, :] + part_recv[part, :].astype(F32)).astype(BF16)
        for i in sorted(range(PER * g, PER * g + PER), key=lambda i: -hops(i)):
            if i:
                to_source(i).start()
            else:
                back[0:SLOTS, :] = back_send[0:SLOTS, :]

    last = None
    for g in order:
        part = slice(HALF * g, HALF * g + HALF)
        for i in range(PER * g, PER * g + PER):
            if i:
                to_expert(i).wait_recv()
        to_partner(xa, xb, fwd_s, fwd_r, g).start()
        if last is not None:
            finish(last)
        to_partner(xa, xb, fwd_s, fwd_r, g).wait_recv()
        block = jnp.concatenate([xa[part, :], xb[part, :]], axis=0)
        gate = jnp.dot(block, wg_v[...], preferred_element_type=F32)
        up = jnp.dot(block, wu_v[...], preferred_element_type=F32)
        hidden = (gate * jax.nn.sigmoid(gate) * up).astype(BF16)
        result = jnp.dot(hidden, wd_v[...], preferred_element_type=F32)
        part_send[part, :] = result[HALF:, :].astype(BF16)
        to_partner(part_send, part_recv, part_s, part_r, g).start()
        own_part[part, :] = result[:HALF, :]
        last = g
    finish(last)

    total = None
    for g in order:
        part = slice(HALF * g, HALF * g + HALF)
        for i in range(PER * g, PER * g + PER):
            if i:
                to_source(i).wait_recv()
        rows = back[part, :]
        more = jnp.dot(high[:, part], rows, preferred_element_type=F32)
        more = more + jnp.dot(low[:, part], rows, preferred_element_type=F32)
        total = more if total is None else total + more
    mixed[...] = (after + rms(total, glast_v[...])).astype(BF16)

    for i in range(1, CHIPS):
        to_expert(i).wait_send()
        to_source(i).wait_send()
    for g in range(GROUPS):
        to_partner(xa, xb, fwd_s, fwd_r, g).wait_send()
        to_partner(part_send, part_recv, part_s, part_r, g).wait_send()


def body(
    tokens, gain_mix, w_query, w_key, w_value, w_input_gate, w_forget_gate, bias_input, bias_forget, memory_cells,
    normalizer, stabilizer, w_mix_out, gain_mix_post, gain_ffn, w_router, routing, w_expert_gate, w_expert_up,
    w_expert_down, gain_ffn_post,
):
    rows, width = tokens.shape
    _, heads, dk, dv = memory_cells.shape
    hidden = w_expert_gate.shape[2]
    row = lambda v: v.reshape(1, -1)
    hbm, vmem = pl.BlockSpec(memory_space=pltpu.HBM), pl.BlockSpec(memory_space=pltpu.VMEM)
    shape = jax.ShapeDtypeStruct
    dma = pltpu.SemaphoreType.DMA
    like = lambda a: pltpu.VMEM(a.shape, a.dtype)
    front_in = (
        tokens, row(gain_mix), w_query, w_key, w_value, w_input_gate.T, w_forget_gate.T, row(bias_input),
        row(bias_forget), memory_cells, normalizer, stabilizer.T,
    )
    cells_next, norm_next, stab_next, cell = pl.pallas_call(
        front_kernel,
        out_shape=(
            shape(memory_cells.shape, F32), shape(normalizer.shape, F32), shape((heads, rows), F32),
            shape((heads, rows, dv), BF16),
        ),
        in_specs=[hbm] * len(front_in),
        out_specs=(hbm, vmem, vmem, hbm),
        scratch_shapes=[like(a) for a in front_in]
        + [
            pltpu.VMEM((heads, rows, dv), BF16),
            pltpu.VMEM((heads * dk, 128), F32), pltpu.VMEM((rows // CHUNK, heads, 8, 128), F32),
            pltpu.VMEM((rows, heads, 256), F32), pltpu.VMEM((rows, heads, 128), F32), pltpu.VMEM((rows, heads, 128), F32),
            pltpu.VMEM((rows, heads, 256), F32), pltpu.VMEM((rows, heads * 128), F32), pltpu.VMEM((128, 128), F32),
            dma((12,)), dma((rows // CHUNK,)), dma((rows // CHUNK,)),
        ],
        compiler_params=pltpu.CompilerParams(vmem_limit_bytes=VMEM_LIMIT),
        name="front",
    )(*front_in)

    big = pltpu.VMEM((LANES, width), BF16)
    router = w_router.T
    mixed = pl.pallas_call(
        expert_kernel,
        out_shape=pltpu.VMEM((rows, width), BF16),
        in_specs=[hbm] * 11,
        out_specs=vmem,
        scratch_shapes=[
            pltpu.VMEM((heads, rows, dv), BF16), like(tokens), like(w_mix_out), like(row(gain_mix_post)), like(row(gain_ffn)), like(router),
            pltpu.VMEM((2, 128), jnp.int32), like(row(gain_ffn_post)), pltpu.VMEM((128, 128), F32),
            pltpu.VMEM((width, hidden), BF16), pltpu.VMEM((width, hidden), BF16), pltpu.VMEM((hidden, width), BF16),
            big, big, big, pltpu.VMEM((LANES, width), F32), big, big, big, big,
            dma((11,)), dma((CHIPS,)), dma((CHIPS,)), dma((GROUPS,)), dma((GROUPS,)), dma((GROUPS,)), dma((GROUPS,)),
            dma((CHIPS,)), dma((CHIPS,)),
        ],
        compiler_params=pltpu.CompilerParams(collective_id=0, has_side_effects=True, vmem_limit_bytes=VMEM_LIMIT - 256 * 1024),
        name="experts",
    )(
        cell, tokens, w_mix_out, row(gain_mix_post), row(gain_ffn), router, routing.T, w_expert_gate, w_expert_up,
        w_expert_down, row(gain_ffn_post),
    )
    return (mixed, cells_next, norm_next, stab_next.T)


def solution(mesh):
    return jax.shard_map(
        body,
        mesh=mesh,
        in_specs=(
            P("ep", None),
            P(),
            P(),
            P(),
            P(),
            P(),
            P(),
            P(),
            P(),
            P("ep", None, None, None),
            P("ep", None, None),
            P("ep", None),
            P(),
            P(),
            P(),
            P(),
            P(),
            P("ep", None, None),
            P("ep", None, None),
            P("ep", None, None),
            P(),
        ),
        out_specs=(P("ep", None), P("ep", None, None, None), P("ep", None, None), P("ep", None)),
        check_vma=False,
    )
```
